32 devices in a mesh: grp: 2 (over y), fs: 4 (over z), tp: 4 (over x, core).
Axes of the slice: x: 2, y: 2, z: 4, core: 2. Of those that a mesh axis runs over, the one named last changes fastest.
Arguments:
- tokens: bfloat16 [2048, 3072], P(('grp', 'tp')), parts along dimension 0, may hold values from -6 to 6
- up_master: float32 [3072, 12288], P('fs', 'tp'), may hold values from -0.109375 to 0.109375
- down_master: float32 [12288, 3072], P('fs', 'tp'), may hold values from -0.0546875 to 0.0546875
- norm_gain: float32 [3072], P('fs'), may hold values from 0.1 to 1.9
Outputs:
- prompt_out: bfloat16 [2048, 3072], P(('grp', 'tp'), 'fs'), parts along dimension 0
- sampled_up: bfloat16 [6144, 12288], P('grp', 'fs'), parts along dimension 0
- sampled_down: bfloat16 [24576, 3072], P(('grp', 'fs')), parts along dimension 0
The draws below stay inside these ranges and needn't reach their ends.
There are 2 independent parts, one for each index of `grp`. The reference program is written for one: setup_inputs(seed, part) draws one part's arguments, and reference() takes and returns one part's arrays. A program takes and returns all parts, laid end to end along the dimension named above; an argument that names none is the same for every part. Nothing has to cross between parts.
All inputs are finite; a program needn't handle non-finite values.
Results may differ from the reference program's by a relative error of at most 0.0074.
Values may be sent and summed in bfloat16 or wider, within the bound.
A program may use at most 192 MiB of HBM per device.

```python
import jax
import jax.numpy as jnp
from jax import lax

D = 3072
FF = 12288
TOKENS = 1024


def block_levels(own_key, shape, split, low, high):
    level = 1.0
    for position, parts in split:
        steps = jax.random.uniform(jax.random.fold_in(jax.random.fold_in(own_key, 6), position), (parts,), jnp.float32, low / len(split), high / len(split))
        level = level * jnp.repeat(jnp.exp(steps), shape[position] // parts).reshape((-1,) + (1,) * (len(shape) - 1 - position))
    return level


def normal_values(key, shape, scale, limit, split=(), held_as=jnp.bfloat16):
    factor_of = block_levels(key, shape, split, -0.22, 0.18) if split else 1.0
    array = jax.random.normal(key, shape, jnp.float32) * scale * factor_of
    return jnp.minimum(jnp.maximum(array, -limit), limit).astype(held_as)


def setup_inputs(seed: int = 0, part: int = 0) -> dict:
    keys = jax.random.split(jax.random.key(seed), 5)
    own_keys = jax.random.split(jax.random.fold_in(keys[4], part), 5)
    return {
        "tokens": normal_values(own_keys[0], (TOKENS, D), 1.0, 6.0, ((0, 4),)),
        "up_master": normal_values(keys[1], (D, FF), D ** -0.5, 0.109375, ((0, 4), (1, 4)), jnp.float32),
        "down_master": normal_values(keys[2], (FF, D), FF ** -0.5, 0.0546875, ((0, 4), (1, 4)), jnp.float32),
        "norm_gain": jnp.clip(1.0 + 0.18 * jax.random.normal(keys[3], (D,), jnp.float32), 0.1, 1.9),
    }


def reference(tokens, up_master, down_master, norm_gain):
    sampled_up = (norm_gain[:, None] * up_master).astype(jnp.bfloat16)
    sampled_down = down_master.astype(jnp.bfloat16)
    values = tokens.astype(jnp.float32)
    center = lax.optimization_barrier(jnp.mean(values, axis=-1, keepdims=True))
    spread = lax.optimization_barrier(jnp.mean(jnp.square(values - center), axis=-1, keepdims=True))
    normalized = ((values - center) * lax.rsqrt(spread + 1e-05)).astype(jnp.bfloat16)
    before = jnp.dot(normalized, sampled_up, preferred_element_type=jnp.float32)
    hidden = jnp.square(jax.nn.relu(before)).astype(jnp.bfloat16)
    prompt_out = jnp.dot(hidden, sampled_down, preferred_element_type=jnp.float32).astype(jnp.bfloat16)
    return (prompt_out, sampled_up, sampled_down)
```

```python
import functools

import jax
import jax.numpy as jnp
from jax import lax
from jax.experimental import pallas as pl
from jax.experimental.pallas import tpu as pltpu
from jax.sharding import PartitionSpec as P

MESH = pl.DeviceIdType.MESH
CORES = 2
LAG = 2


def normalize(tokens):
    values = tokens.astype(jnp.float32)
    center = jnp.mean(values, axis=-1, keepdims=True)
    spread = jnp.mean(jnp.square(values - center), axis=-1, keepdims=True)
    return ((values - center) * lax.rsqrt(spread + 1e-05)).astype(jnp.bfloat16)


def pieces_of(size, unit, most):
    for count in range(most, 1, -1):
        if size % (count * unit) == 0:
            return count
    return 1


def hand_over(dims, cuts, up_ref, down_ref, got_up, got_down, up_room, down_room, up_sems, down_sems, room_sem):
    groups, fs, tp = dims
    pairs = tp // CORES
    up_cuts, down_cuts = cuts
    y, f, t = lax.axis_index("grp"), lax.axis_index("fs"), lax.axis_index("tp")
    x, k = t // CORES, t % CORES
    blocks = up_ref.shape[0]
    first_send, first_recv, x_send, y_send, y_recv, a_send, a_recv, b_send, b_recv = up_sems
    own_send, own_recv, dx_send, dx_recv, dy_send, dy_recv, da_send, da_recv, db_send, db_recv = down_sems
    cols = up_ref.shape[3] // up_cuts
    home = (f // blocks) // CORES
    sibling = (y, f, x * CORES + (1 - k))

    def remote(src, dst, send, recv, where):
        return pltpu.make_async_remote_copy(src_ref=src, dst_ref=dst, send_sem=send, recv_sem=recv, device_id=where, device_id_type=MESH)

    height = down_ref.shape[0] // (groups * down_cuts)
    width = down_ref.shape[1]

    def down_at(ref, group, cut, column):
        return ref.at[pl.ds(pl.multiple_of((group * down_cuts + cut) * height, height), height), pl.ds(pl.multiple_of(column * width, width), width)]

    def down_first(dx, cut):
        xo = (x + dx) % pairs
        return remote(down_at(down_ref, y, cut, 0), down_at(got_down, y, cut, t), dx_send.at[dx - 1, cut], dx_recv.at[dx - 1, cut], (y, f, xo * CORES + k))

    def down_y(dx, dy, cut):
        column = ((x - dx + pairs) % pairs) * CORES + k
        here = down_at(got_down, y, cut, column)
        return remote(here, here, dy_send.at[dx - 1, dy - 1, cut], dy_recv.at[dx - 1, dy - 1, cut], ((y + dy) % groups, f, t))

    def down_a(dx, cut):
        column = ((x - dx + pairs) % pairs) * CORES + k
        here = down_at(got_down, y, cut, column)
        return remote(here, here, da_send.at[dx - 1, cut], da_recv.at[dx - 1, cut], sibling)

    def down_b(dx, dy, cut):
        column = ((x - dx + pairs) % pairs) * CORES + k
        here = down_at(got_down, (y - dy + groups) % groups, cut, column)
        return remote(here, here, db_send.at[dx - 1, dy - 1, cut], db_recv.at[dx - 1, dy - 1, cut], sibling)

    own_columns = got_down.at[:, pl.ds(pl.multiple_of(t * width, width), width)]
    down_own = remote(down_ref, own_columns, own_send, own_recv, sibling)

    def up_at(ref, block, group, lane, cut):
        return ref.at[block, group * CORES + lane, :, pl.ds(cut * cols, cols)]

    def up_first(block, lane, cut):
        to = t * blocks + block
        return remote(up_at(up_ref, block, y, lane, cut), up_at(got_up, f, y, lane, cut), first_send.at[block, lane, cut], first_recv.at[f, cut], (y, to, x * CORES + lane))

    def up_x(r, cut, dx):
        here = up_at(got_up, r, y, k, cut)
        return remote(here, here, x_send.at[dx - 1, r, cut], first_recv.at[r, cut], (y, f, ((x + dx) % pairs) * CORES + k))

    def up_y(r, cut, dy):
        here = up_at(got_up, r, y, k, cut)
        return remote(here, here, y_send.at[dy - 1, r, cut], y_recv.at[dy - 1, r, cut], ((y + dy) % groups, f, t))

    def up_a(r, cut):
        here = up_at(got_up, r, y, k, cut)
        return remote(here, here, a_send.at[r, cut], a_recv.at[r, cut], sibling)

    def up_b(r, cut, dy):
        here = up_at(got_up, r, (y - dy + groups) % groups, k, cut)
        return remote(here, here, b_send.at[dy - 1, r, cut], b_recv.at[dy - 1, r, cut], sibling)

    def is_self(block, lane):
        return jnp.logical_and(t * blocks + block == f, lane == k)

    room_in = pltpu.make_async_copy(up_ref.at[f % blocks, y * CORES + k], up_room, room_sem.at[0])
    down_in = pltpu.make_async_copy(down_ref, down_room, room_sem.at[1])
    down_out = pltpu.make_async_copy(down_room, own_columns, room_sem.at[2])

    def room_out(cut):
        return pltpu.make_async_copy(up_room.at[:, pl.ds(cut * cols, cols)], up_at(got_up, f, y, k, cut), first_recv.at[f, cut])

    room_in.start()
    down_in.start()
    for cut in range(down_cuts):
        for dx in range(1, pairs):
            down_first(dx, cut).start()
    for cut in range(up_cuts):
        for block in range(blocks):
            for lane in range(CORES):
                @pl.when(jnp.logical_not(is_self(block, lane)))
                def _():
                    up_first(block, lane, cut).start()
    down_own.start()
    room_in.wait()
    owner = f // blocks == t

    @pl.when(owner)
    def _():
        for cut in range(up_cuts):
            room_out(cut).start()

    down_in.wait()
    down_out.start()

    for step in range(down_cuts + LAG):
        if step < down_cuts:
            for dx in range(1, pairs):
                down_first(dx, step).wait_recv()
                for dy in range(1, groups):
                    down_y(dx, dy, step).start()
                down_a(dx, step).start()
        if step >= LAG:
            for dx in range(1, pairs):
                for dy in range(1, groups):
                    down_y(dx, dy, step - LAG).wait_recv()
                    down_b(dx, dy, step - LAG).start()

    def up_arrival(step):
        cut, r = step // fs, (f + step) % fs
        pltpu.make_async_copy(up_at(got_up, r, y, k, cut), up_at(got_up, r, y, k, cut), first_recv.at[r, cut]).wait()

        @pl.when(x == home)
        def _():
            for dx in range(1, pairs):
                up_x(r, cut, dx).start()

        for dy in range(1, groups):
            up_y(r, cut, dy).start()
        up_a(r, cut).start()

    def up_second(step):
        cut, r = step // fs, (f + step) % fs
        for dy in range(1, groups):
            up_y(r, cut, dy).wait_recv()
            up_b(r, cut, dy).start()

    for step in range(up_cuts * fs + LAG):
        if step < up_cuts * fs:
            up_arrival(step)
        if step >= LAG:
            up_second(step - LAG)

    for cut in range(up_cuts):
        for r in range(fs):
            up_a(r, cut).wait()
            for dy in range(1, groups):
                up_b(r, cut, dy).wait()
                up_y(r, cut, dy).wait_send()

            @pl.when(x == home)
            def _():
                for dx in range(1, pairs):
                    up_x(r, cut, dx).wait_send()

        for block in range(blocks):
            for lane in range(CORES):
                @pl.when(jnp.logical_not(is_self(block, lane)))
                def _():
                    up_first(block, lane, cut).wait_send()
    for cut in range(down_cuts):
        for dx in range(1, pairs):
            down_first(dx, cut).wait_send()
            down_a(dx, cut).wait()
            for dy in range(1, groups):
                down_y(dx, dy, cut).wait_send()
                down_b(dx, dy, cut).wait()
    down_own.wait()
    down_out.wait()


def gather(up_cast, down_cast, dims):
    groups, fs, tp = dims
    rows, cols = up_cast.shape[0] // (groups * CORES), up_cast.shape[1] * tp // fs
    blocks = fs // tp
    by_block = up_cast.reshape(groups * CORES, rows, blocks, cols).transpose(2, 0, 1, 3)
    height, width = down_cast.shape
    up_cuts = pieces_of(cols, 128, 4)
    down_cuts = pieces_of(height // groups, 16, 8)
    pairs = tp // CORES
    dma = pltpu.SemaphoreType.DMA
    up_sems = [
        dma((blocks, CORES, up_cuts)),
        dma((fs, up_cuts)),
        dma((pairs - 1, fs, up_cuts)),
        dma((groups - 1, fs, up_cuts)),
        dma((groups - 1, fs, up_cuts)),
        dma((fs, up_cuts)),
        dma((fs, up_cuts)),
        dma((groups - 1, fs, up_cuts)),
        dma((groups - 1, fs, up_cuts)),
    ]
    one, two = (pairs - 1, down_cuts), (pairs - 1, groups - 1, down_cuts)
    down_sems = [dma, dma, dma(one), dma(one), dma(two), dma(two), dma(one), dma(one), dma(two), dma(two)]
    got_up, got_down = pl.pallas_call(
        functools.partial(hand_over, dims, (up_cuts, down_cuts)),
        out_shape=(
            jax.ShapeDtypeStruct((fs, groups * CORES, rows, cols), jnp.bfloat16),
            jax.ShapeDtypeStruct((height, tp * width), jnp.bfloat16),
        ),
        in_specs=[pl.BlockSpec(memory_space=pl.ANY)] * 2,
        out_specs=(pl.BlockSpec(memory_space=pl.ANY),) * 2,
        scratch_shapes=[
            pltpu.VMEM((rows, cols), jnp.bfloat16),
            pltpu.VMEM((height, width), jnp.bfloat16),
            up_sems,
            down_sems,
            dma((3,)),
        ],
        compiler_params=pltpu.CompilerParams(has_side_effects=True),
    )(by_block, down_cast)
    return got_up.reshape(fs * groups * CORES * rows, cols), got_down


def shards(dims, tokens, up_master, down_master, norm_gain):
    up_cast = (norm_gain[:, None] * up_master).astype(jnp.bfloat16)
    down_cast = down_master.astype(jnp.bfloat16)
    sampled_up, sampled_down = gather(up_cast, down_cast, dims)
    normalized = normalize(tokens)
    before = jnp.dot(normalized, sampled_up, preferred_element_type=jnp.float32)
    hidden = jnp.square(jax.nn.relu(before)).astype(jnp.bfloat16)
    terms = jnp.dot(hidden, sampled_down, preferred_element_type=jnp.float32)
    summed = lax.psum_scatter(terms, "fs", scatter_dimension=1, tiled=True)
    return (summed.astype(jnp.bfloat16), sampled_up, sampled_down)


def solution(mesh):
    dims = tuple(mesh.shape[name] for name in ("grp", "fs", "tp"))
    return jax.shard_map(
        functools.partial(shards, dims),
        mesh=mesh,
        in_specs=(P(("grp", "tp"), None), P("fs", "tp"), P("fs", "tp"), P("fs")),
        out_specs=(P(("grp", "tp"), "fs"), P("grp", "fs"), P(("grp", "fs"), None)),
        check_vma=False,
    )
```

```python
import functools

import jax
import jax.numpy as jnp
from jax import lax
from jax.experimental import pallas as pl
from jax.experimental.pallas import tpu as pltpu
from jax.sharding import PartitionSpec as P

MESH = pl.DeviceIdType.MESH
CORES = 2
LAG = 2
EARLY = 2
UNIT = 256
LIMIT = 14


def normalize(tokens):
    values = tokens.astype(jnp.float32)
    center = jnp.mean(values, axis=-1, keepdims=True)
    spread = jnp.mean(jnp.square(values - center), axis=-1, keepdims=True)
    return ((values - center) * lax.rsqrt(spread + 1e-05)).astype(jnp.bfloat16)


def pieces_of(size, unit, most):
    for count in range(most, 1, -1):
        if size % (count * unit) == 0:
            return count
    return 1


def hand_over(dims, cuts, rows_ref, up_ref, down_ref, got_up, got_down, out_ref, hidden, mine, sent, landed, up_sems, down_sems, sum_sems, local_sem):
    groups, fs, tp = dims
    pairs = tp // CORES
    up_cuts, down_cuts = cuts
    y, f, t = lax.axis_index("grp"), lax.axis_index("fs"), lax.axis_index("tp")
    x, k = t // CORES, t % CORES
    first_send, first_recv, x_send, y_send, y_recv, a_send, a_recv, b_send, b_recv = up_sems
    own_send, own_recv, dx_send, dx_recv, dy_send, dy_recv, da_send, da_recv, db_send, db_recv = down_sems
    sum_send, sum_recv = sum_sems
    cols = up_ref.shape[2] // up_cuts
    depth = got_up.shape[0] * got_up.shape[1] * got_up.shape[2]
    home = f // CORES
    sibling = (y, f, x * CORES + (1 - k))

    def remote(src, dst, send, recv, where):
        return pltpu.make_async_remote_copy(src_ref=src, dst_ref=dst, send_sem=send, recv_sem=recv, device_id=where, device_id_type=MESH)

    height = down_ref.shape[0] // groups
    width = down_ref.shape[1]
    tile = width // down_cuts

    def down_at(ref, group, cut, column):
        return ref.at[pl.ds(pl.multiple_of(group * height, height), height), pl.ds(pl.multiple_of(column * width + cut * tile, tile), tile)]

    def from_pair(dx):
        return ((x - dx + pairs) % pairs) * CORES + k

    def down_first(dx, cut):
        return remote(down_at(down_ref, y, cut, 0), down_at(got_down, y, cut, t), dx_send.at[dx - 1, cut], dx_recv.at[dx - 1, cut], (y, f, ((x + dx) % pairs) * CORES + k))

    def down_y(dx, dy, cut):
        here = down_at(got_down, y, cut, from_pair(dx))
        return remote(here, here, dy_send.at[dx - 1, dy - 1, cut], dy_recv.at[dx - 1, dy - 1, cut], ((y + dy) % groups, f, t))

    def down_a(dx, cut):
        here = down_at(got_down, y, cut, from_pair(dx))
        return remote(here, here, da_send.at[dx - 1, cut], da_recv.at[dx - 1, cut], sibling)

    def down_b(dx, dy, cut):
        here = down_at(got_down, (y - dy + groups) % groups, cut, from_pair(dx))
        return remote(here, here, db_send.at[dx - 1, dy - 1, cut], db_recv.at[dx - 1, dy - 1, cut], sibling)

    own_columns = got_down.at[:, pl.ds(pl.multiple_of(t * width, width), width)]
    down_own = remote(down_ref, own_columns, own_send, own_recv, sibling)
    down_here = pltpu.make_async_copy(down_ref, own_columns, local_sem)

    def up_at(ref, group, lane, cut):
        return ref.at[group * CORES + lane, :, pl.ds(cut * cols, cols)]

    def up_first(lane, cut):
        return remote(up_at(up_ref, y, lane, cut), up_at(got_up.at[f], y, lane, cut), first_send.at[lane, cut], first_recv.at[f, cut], (y, t, x * CORES + lane))

    def up_here(r, cut):
        return pltpu.make_async_copy(up_at(up_ref, y, k, cut), up_at(got_up.at[r], y, k, cut), first_recv.at[r, cut])

    def up_x(r, cut, dx):
        here = up_at(got_up.at[r], y, k, cut)
        return remote(here, here, x_send.at[dx - 1, r, cut], first_recv.at[r, cut], (y, f, ((x + dx) % pairs) * CORES + k))

    def up_y(r, cut, dy):
        here = up_at(got_up.at[r], y, k, cut)
        return remote(here, here, y_send.at[dy - 1, r, cut], y_recv.at[dy - 1, r, cut], ((y + dy) % groups, f, t))

    def up_a(r, cut):
        here = up_at(got_up.at[r], y, k, cut)
        return remote(here, here, a_send.at[r, cut], a_recv.at[r, cut], sibling)

    def up_b(r, cut, dy):
        here = up_at(got_up.at[r], (y - dy + groups) % groups, k, cut)
        return remote(here, here, b_send.at[dy - 1, r, cut], b_recv.at[dy - 1, r, cut], sibling)

    def is_self(lane):
        return jnp.logical_and(t == f, lane == k)

    def hidden_units(cut):
        @pl.loop(0, cols // UNIT)
        def _(step):
            at = pl.ds(pl.multiple_of(cut * cols + step * UNIT, UNIT), UNIT)
            block = got_up[:, :, :, at].reshape(depth, UNIT)
            before = jnp.dot(rows_ref[...], block, preferred_element_type=jnp.float32)
            hidden[:, at] = jnp.square(jnp.maximum(before, 0.0)).astype(jnp.bfloat16)

    def sum_to(column, cut):
        at = pl.ds(cut * tile, tile)
        return remote(sent.at[column, :, at], landed.at[f, :, at], sum_send.at[column, cut], sum_recv.at[f, cut], (y, column, t))

    def features(column, cut):
        at = pl.ds(pl.multiple_of(column * width + cut * tile, tile), tile)
        term = jnp.dot(hidden[...], got_down[:, at], preferred_element_type=jnp.float32)

        @pl.when(column == f)
        def _():
            mine[:, pl.ds(cut * tile, tile)] = term

        @pl.when(column != f)
        def _():
            sent[column, :, pl.ds(cut * tile, tile)] = term.astype(jnp.bfloat16)
            sum_to(column, cut).start()

    early = min(EARLY, down_cuts)
    for lane in range(CORES):
        @pl.when(is_self(lane))
        def _():
            for cut in range(up_cuts):
                up_here(f, cut).start()
    for cut in range(early):
        for dx in range(1, pairs):
            down_first(dx, cut).start()
    for cut in range(up_cuts):
        for lane in range(CORES):
            @pl.when(jnp.logical_not(is_self(lane)))
            def _():
                up_first(lane, cut).start()
    down_here.start()
    down_own.start()

    @pl.when(x != home)
    def _():
        for cut in range(early, down_cuts):
            for dx in range(1, pairs):
                down_first(dx, cut).start()

    order = [(0, cut) for cut in range(up_cuts)] + [(j, cut) for cut in range(up_cuts) for j in range(1, fs)]

    def up_arrival(j, cut):
        r = (f + j) % fs
        up_here(r, cut).wait()

        @pl.when(x == home)
        def _():
            for dx in range(1, pairs):
                up_x(r, cut, dx).start()

        for dy in range(1, groups):
            up_y(r, cut, dy).start()
        up_a(r, cut).start()

    def up_second(j, cut):
        r = (f + j) % fs
        for dy in range(1, groups):
            up_y(r, cut, dy).wait_recv()
            up_b(r, cut, dy).start()

    def up_done(cut):
        for j in range(fs):
            r = (f + j) % fs
            up_a(r, cut).wait_recv()
            for dy in range(1, groups):
                up_b(r, cut, dy).wait_recv()
        hidden_units(cut)

    done = 0
    for step in range(len(order) + LAG):
        if step < len(order):
            up_arrival(*order[step])
        if step == len(order) - 1:
            @pl.when(x == home)
            def _():
                for cut in range(early, down_cuts):
                    for dx in range(1, pairs):
                        down_first(dx, cut).start()
        if step >= LAG:
            up_second(*order[step - LAG])
        if done < up_cuts - 1 and step == up_cuts + (done + 2) * (fs - 1) - 1:
            up_done(done)
            done += 1

    down_here.wait()
    for step in range(down_cuts + 2):
        if step < down_cuts:
            for dx in range(1, pairs):
                down_first(dx, step).wait_recv()
                for dy in range(1, groups):
                    down_y(dx, dy, step).start()
                down_a(dx, step).start()
        if step == 0:
            for cut in range(done, up_cuts):
                up_done(cut)
        if 1 <= step <= down_cuts:
            for dx in range(1, pairs):
                for dy in range(1, groups):
                    down_y(dx, dy, step - 1).wait_recv()
                    down_b(dx, dy, step - 1).start()
        if step < down_cuts:
            features(t, step)
            if step == 0:
                down_own.wait_recv()
            features(x * CORES + (1 - k), step)
        if 1 <= step <= down_cuts:
            for dx in range(1, pairs):
                features(from_pair(dx), step - 1)
        if step >= 2:
            for dx in range(1, pairs):
                down_a(dx, step - 2).wait_recv()
                for dy in range(1, groups):
                    down_b(dx, dy, step - 2).wait_recv()
                features(((x - dx + pairs) % pairs) * CORES + (1 - k), step - 2)

    for cut in range(down_cuts):
        at = pl.ds(cut * tile, tile)
        for j in range(1, fs):
            r = (f + j) % fs
            remote(sent.at[r, :, at], landed.at[r, :, at], sum_send.at[r, cut], sum_recv.at[r, cut], (y, r, t)).wait_recv()
        total = mine[:, at]
        for j in range(1, fs):
            total += landed[(f + j) % fs, :, at].astype(jnp.float32)
        out_ref[:, at] = total.astype(jnp.bfloat16)

    for cut in range(up_cuts):
        for j in range(fs):
            r = (f + j) % fs
            up_a(r, cut).wait_send()
            for dy in range(1, groups):
                up_b(r, cut, dy).wait_send()
                up_y(r, cut, dy).wait_send()

            @pl.when(x == home)
            def _():
                for dx in range(1, pairs):
                    up_x(r, cut, dx).wait_send()

        for lane in range(CORES):
            @pl.when(jnp.logical_not(is_self(lane)))
            def _():
                up_first(lane, cut).wait_send()
    for cut in range(down_cuts):
        for dx in range(1, pairs):
            down_first(dx, cut).wait_send()
            down_a(dx, cut).wait_send()
            for dy in range(1, groups):
                down_y(dx, dy, cut).wait_send()
                down_b(dx, dy, cut).wait_send()
        for j in range(1, fs):
            sum_to((f + j) % fs, cut).wait_send()
    down_own.wait_send()


def fused(rows_in, up_cast, down_cast, dims):
    groups, fs, tp = dims
    rows, cols = up_cast.shape[0] // (groups * CORES), up_cast.shape[1]
    height, width = down_cast.shape
    tokens = rows_in.shape[0]
    up_cuts = pieces_of(cols, UNIT, 4)
    down_cuts = pieces_of(width, 128, 6)
    pairs = tp // CORES
    dma = pltpu.SemaphoreType.DMA
    far = groups - 1
    up_sems = [dma((CORES, up_cuts)), dma((fs, up_cuts)), dma((pairs - 1, fs, up_cuts)), dma((far, fs, up_cuts)), dma((far, fs, up_cuts))]
    up_sems += [dma((fs, up_cuts)), dma((fs, up_cuts)), dma((far, fs, up_cuts)), dma((far, fs, up_cuts))]
    one, two = (pairs - 1, down_cuts), (pairs - 1, far, down_cuts)
    down_sems = [dma, dma, dma(one), dma(one), dma(two), dma(two), dma(one), dma(one), dma(two), dma(two)]
    vmem = pl.BlockSpec(memory_space=pltpu.VMEM)
    hbm = pl.BlockSpec(memory_space=pl.ANY)
    got_up, got_down, out = pl.pallas_call(
        functools.partial(hand_over, dims, (up_cuts, down_cuts)),
        out_shape=(
            pltpu.VMEM((fs, groups * CORES, rows, cols), jnp.bfloat16),
            pltpu.VMEM((height, tp * width), jnp.bfloat16),
            jax.ShapeDtypeStruct((tokens, width), jnp.bfloat16),
        ),
        in_specs=[vmem, hbm, hbm],
        out_specs=(vmem, vmem, vmem),
        scratch_shapes=[
            pltpu.VMEM((tokens, cols), jnp.bfloat16),
            pltpu.VMEM((tokens, width), jnp.float32),
            pltpu.VMEM((fs, tokens, width), jnp.bfloat16),
            pltpu.VMEM((fs, tokens, width), jnp.bfloat16),
            up_sems,
            down_sems,
            [dma((fs, down_cuts)), dma((fs, down_cuts))],
            dma,
        ],
        compiler_params=pltpu.CompilerParams(has_side_effects=True, vmem_limit_bytes=LIMIT << 20),
    )(rows_in, up_cast.reshape(groups * CORES, rows, cols), down_cast)
    return out, got_up.reshape(fs * groups * CORES * rows, cols), got_down


def fits(up_shape, down_shape, dims):
    groups, fs, tp = dims
    own = 2 * (up_shape[0] * up_shape[1] * fs + down_shape[0] * down_shape[1] * tp)
    aligned = up_shape[0] % (groups * CORES * 16) == 0 and up_shape[1] % UNIT == 0
    return fs == tp and groups > 1 and tp % CORES == 0 and tp > CORES and aligned and down_shape[0] % (groups * 16) == 0 and down_shape[1] % 128 == 0 and own <= 40 << 20


def by_collectives(normalized, up_cast, down_cast):
    quarter = lax.all_to_all(up_cast, "tp", split_axis=0, concat_axis=1, tiled=True)
    moved = lax.all_to_all(quarter, "fs", split_axis=1, concat_axis=0, tiled=True)
    part_rows = quarter.shape[0]
    stacked = moved.reshape(moved.shape[0] // part_rows, part_rows, moved.shape[1])
    joined = lax.all_gather(stacked, "tp", axis=1, tiled=True)
    sampled_down = lax.all_gather(down_cast, "tp", axis=1, tiled=True)
    sampled_up = joined.reshape(joined.shape[0] * joined.shape[1], joined.shape[2])
    before = jnp.dot(normalized, sampled_up, preferred_element_type=jnp.float32)
    hidden = jnp.square(jax.nn.relu(before)).astype(jnp.bfloat16)
    terms = jnp.dot(hidden, sampled_down, preferred_element_type=jnp.float32)
    summed = lax.psum_scatter(terms, "fs", scatter_dimension=1, tiled=True)
    return summed.astype(jnp.bfloat16), sampled_up, sampled_down


def shards(dims, tokens, up_master, down_master, norm_gain):
    up_cast = (norm_gain[:, None] * up_master).astype(jnp.bfloat16)
    down_cast = down_master.astype(jnp.bfloat16)
    normalized = normalize(tokens)
    if fits(up_master.shape, down_master.shape, dims):
        return fused(normalized, up_cast, down_cast, dims)
    return by_collectives(normalized, up_cast, down_cast)


def solution(mesh):
    dims = tuple(mesh.shape[name] for name in ("grp", "fs", "tp"))
    return jax.shard_map(
        functools.partial(shards, dims),
        mesh=mesh,
        in_specs=(P(("grp", "tp"), None), P("fs", "tp"), P("fs", "tp"), P("fs")),
        out_specs=(P(("grp", "tp"), "fs"), P("grp", "fs"), P(("grp", "fs"), None)),
        check_vma=False,
    )
```
